32 devices in a mesh: ep: 8 (over z, x), tp: 4 (over y, core).
Axes of the slice: x: 2, y: 2, z: 4, core: 2. Of those that a mesh axis runs over, the one named last changes fastest.
Arguments:
- conv_value: bfloat16 [1024, 4096], P('tp', 'ep'), may hold values from -6 to 6
- conv_gate: bfloat16 [1024, 4096], P('tp', 'ep'), may hold values from -8 to 8
- conv_kernel: bfloat16 [31, 1024], P(None, 'tp'), may hold values from -1 to 1
- norm_gain: float32 [1024], replicated, may hold values from 0.1 to 1.9
- norm_shift: float32 [1024], replicated, may hold values from -3 to 3
- out_weight: bfloat16 [1024, 4096], P(None, 'tp'), may hold values from -0.1875 to 0.1875
- expert_input: bfloat16 [1024, 4096], P('ep'), may hold values from -6 to 6
- expert_ids: int32 [1024, 2], P('ep'), may hold values from 0 to 7, as said below
- pair_logits: float32 [1024, 2], P('ep'), may hold values from -6 to 6
- group_prob: float32 [1024], P('ep'), may hold values from 0.3 to 1
- expert_gate: bfloat16 [8, 4096, 2048], P('ep', None, 'tp'), may hold values from -0.09375 to 0.09375
- expert_up: bfloat16 [8, 4096, 2048], P('ep', None, 'tp'), may hold values from -0.09375 to 0.09375
- expert_down: bfloat16 [8, 2048, 4096], P('ep', None, 'tp'), may hold values from -0.125 to 0.125
Outputs:
- mixer_out: bfloat16 [4096, 4096], P('ep', 'tp')
- expert_out: bfloat16 [1024, 4096], P('ep', 'tp')
The draws below stay inside these ranges and needn't reach their ends.
Inputs may be any that keep to these rules, and one draw needn't show every extreme that they name: `expert_ids`: the two experts of a token differ and lie in one group, ids g * 2 to (g + 1) * 2 - 1 for some g. The 128 tokens of one index of ep name every expert exactly 32 times.
All inputs are finite; a program needn't handle non-finite values.
Results may differ from the reference program's by a relative error of at most 0.0064.
Values may be sent and summed in bfloat16 or wider, within the bound.
No kernel may reach another device: no remote copies, remote signals or barrier semaphores. Data moves between devices by JAX's collectives and lax.ppermute only.
A program may use at most 64 MiB of HBM per device.

```python
import jax
import jax.numpy as jnp
from jax import lax

D = 4096
CONV_CH = 1024
KERNEL = 31
EXPERT_FF = 2048
GROUPS = 4
B_DEV = 128
EXPERTS = 8
TOK_A = 4096
TOK_B = 1024


def draw_expert_ids(key, part):
    group_size = EXPERTS // GROUPS
    blocks = TOK_B // B_DEV

    def one_block(block_key):
        key_order, key_offset, key_stride = jax.random.split(block_key, 3)
        order = jax.random.permutation(key_order, B_DEV)
        places = jnp.arange(B_DEV, dtype=jnp.int32)
        group = places % GROUPS
        ordinal = places // GROUPS
        offsets = jax.random.randint(key_offset, (GROUPS,), 0, group_size)
        strides = jax.random.randint(key_stride, (GROUPS,), 0, group_size - 1)
        first = (ordinal + offsets[group]) % group_size
        second = (first + 1 + strides[group]) % group_size
        chosen = jnp.stack([group * group_size + first, group * group_size + second], axis=1).astype(jnp.int32)
        return jnp.zeros((B_DEV, 2), jnp.int32).at[order].set(chosen)
    block_keys = jax.random.split(jax.random.fold_in(key, 17), blocks)
    return jax.vmap(one_block)(block_keys).reshape(TOK_B, 2).astype(jnp.int32)


def block_levels(stream_key, dims, shards, low, largest):
    level, own = 1.0, jax.random.fold_in(stream_key, 6)
    for dim, shards_of in shards:
        steps = jnp.exp(jax.random.uniform(jax.random.fold_in(own, dim), (shards_of,), jnp.float32, low / len(shards), largest / len(shards)))
        level = level * jnp.repeat(steps, dims[dim] // shards_of).reshape([-1 if axis == dim else 1 for axis in range(len(dims))])
    return level


def gaussian(stream_key, dims, scale, bound, cuts=(), held_as=jnp.bfloat16):
    factor_of = block_levels(stream_key, dims, cuts, -0.22, 0.18) if cuts else 1.0
    drawn = jax.random.normal(stream_key, dims, jnp.float32) * scale * factor_of
    return jnp.minimum(jnp.maximum(drawn, -bound), bound).astype(held_as)


def setup_inputs(seed: int = 0) -> dict:
    key_of = jax.random.split(jax.random.key(seed), 14)
    return {
        "conv_value": gaussian(key_of[0], (CONV_CH, TOK_A), 1.0, 6.0, ((0, 4), (1, 8))),
        "conv_gate": gaussian(key_of[1], (CONV_CH, TOK_A), 1.5, 8.0, ((0, 4), (1, 8))),
        "conv_kernel": gaussian(key_of[2], (KERNEL, CONV_CH), KERNEL ** -0.5, 1.0, ((1, 4),)),
        "norm_gain": jnp.clip(1.0 + 0.18 * jax.random.normal(key_of[3], (CONV_CH,), jnp.float32), 0.1, 1.9),
        "norm_shift": gaussian(key_of[4], (CONV_CH,), 0.5, 3.0, (), jnp.float32),
        "out_weight": gaussian(key_of[5], (CONV_CH, D), CONV_CH ** -0.5, 0.1875, ((1, 4),)),
        "expert_input": gaussian(key_of[6], (TOK_B, D), 1.0, 6.0, ((0, 8),)),
        "expert_ids": draw_expert_ids(jax.random.fold_in(key_of[13], 71), 0),
        "pair_logits": gaussian(key_of[8], (TOK_B, 2), 1.5, 6.0, ((0, 8),), jnp.float32),
        "group_prob": jnp.clip(0.3 + 0.7 * jax.random.uniform(key_of[9], (TOK_B,), jnp.float32) ** block_levels(key_of[9], (TOK_B,), ((0, 8),), -0.2, 0.2), 0.3, 1.0),
        "expert_gate": gaussian(key_of[10], (EXPERTS, D, EXPERT_FF), D ** -0.5, 0.09375, ((0, 8), (2, 4))),
        "expert_up": gaussian(key_of[11], (EXPERTS, D, EXPERT_FF), D ** -0.5, 0.09375, ((0, 8), (2, 4))),
        "expert_down": gaussian(key_of[12], (EXPERTS, EXPERT_FF, D), EXPERT_FF ** -0.5, 0.125, ((0, 8), (2, 4))),
    }


def norm_swish(conv_out, norm_gain, norm_shift):
    values = conv_out.astype(jnp.float32)
    center = lax.optimization_barrier(jnp.mean(values, axis=0, keepdims=True))
    spread = lax.optimization_barrier(jnp.mean(jnp.square(values - center), axis=0, keepdims=True))
    normed = (values - center) * lax.rsqrt(spread + 1e-05) * norm_gain[:, None] + norm_shift[:, None]
    return jax.nn.silu(normed).astype(jnp.bfloat16)

def route_weights(pair_logits, group_prob):
    share = jax.nn.sigmoid(pair_logits[:, 0] - pair_logits[:, 1])
    return jnp.stack([share, 1.0 - share], axis=1) * group_prob[:, None]

def reference(conv_value, conv_gate, conv_kernel, norm_gain, norm_shift, out_weight, expert_input, expert_ids, pair_logits, group_prob, expert_gate, expert_up, expert_down):
    gated = (conv_value.astype(jnp.float32) * jax.nn.sigmoid(conv_gate.astype(jnp.float32))).astype(jnp.bfloat16)
    reach = (KERNEL - 1) // 2
    length = gated.shape[1]
    padded = jnp.pad(gated.astype(jnp.float32), ((0, 0), (reach, reach)))
    kernel_f = conv_kernel.astype(jnp.float32)
    summed = jnp.zeros(gated.shape, jnp.float32)
    for offset in range(KERNEL):
        summed = summed + kernel_f[offset][:, None] * padded[:, offset:offset + length]
    conv_out = summed.astype(jnp.bfloat16)
    swished = norm_swish(conv_out, norm_gain, norm_shift)
    mixer_out = lax.dot_general(swished, out_weight, (((0,), (0,)), ((), ())), preferred_element_type=jnp.float32).astype(jnp.bfloat16)
    weights = route_weights(pair_logits, group_prob)
    flat = expert_ids.reshape(-1).astype(jnp.int32)
    order = jnp.argsort(flat, stable=True).astype(jnp.int32)
    experts_all = expert_gate.shape[0]
    per_expert = flat.shape[0] // experts_all
    rows = (order // 2).astype(jnp.int32).reshape(experts_all, per_expert)

    def one_expert(packed):
        rows_here, gate_w, up_w, down_w = packed
        block = expert_input[rows_here]
        gate_val = jnp.dot(block, gate_w, preferred_element_type=jnp.float32)
        up_val = jnp.dot(block, up_w, preferred_element_type=jnp.float32)
        hidden = (jax.nn.silu(gate_val) * up_val).astype(jnp.bfloat16)
        return jnp.dot(hidden, down_w, preferred_element_type=jnp.float32).astype(jnp.bfloat16)
    results = lax.map(one_expert, (rows, expert_gate, expert_up, expert_down))
    width = expert_input.shape[1]
    copies = jnp.zeros((flat.shape[0], width), jnp.bfloat16).at[order].set(results.reshape(-1, width))
    copies = copies.reshape(-1, 2, width).astype(jnp.float32)
    expert_out = lax.optimization_barrier(jnp.sum(copies * weights[:, :, None], axis=1)).astype(jnp.bfloat16)
    return (mixer_out, expert_out)
```

```python
import jax
import jax.numpy as jnp
from jax import lax
from jax.sharding import PartitionSpec as P


def extended(cells, sides, width):
    for axis, dim in sides:
        count = lax.axis_size(axis)
        ends = count - 1
        head = lax.slice_in_dim(cells, 0, width, axis=dim)
        tail = lax.slice_in_dim(cells, cells.shape[dim] - width, cells.shape[dim], axis=dim)
        cells = jnp.concatenate(
            [
                lax.ppermute(tail, axis, [(i, (i + 1) % count) for i in range(ends)]),
                cells,
                lax.ppermute(head, axis, [((i + 1) % count, i) for i in range(ends)]),
            ],
            axis=dim,
        )
    return cells


def norm_swish(conv_out, norm_gain, norm_shift):
    values = conv_out.astype(jnp.float32)
    center = jnp.mean(values, axis=0, keepdims=True)
    spread = jnp.mean(jnp.square(values - center), axis=0, keepdims=True)
    normed = (values - center) * lax.rsqrt(spread + 1e-05) * norm_gain[:, None] + norm_shift[
        :, None
    ]
    return jax.nn.silu(normed).astype(jnp.bfloat16)


def route_weights(pair_logits, group_prob):
    share = jax.nn.sigmoid(pair_logits[:, 0] - pair_logits[:, 1])
    return jnp.stack([share, 1.0 - share], axis=1) * group_prob[:, None]


def local(
    conv_value,
    conv_gate,
    conv_kernel,
    norm_gain,
    norm_shift,
    out_weight,
    expert_input,
    expert_ids,
    pair_logits,
    group_prob,
    expert_gate,
    expert_up,
    expert_down,
):
    gated = (conv_value.astype(jnp.float32) * jax.nn.sigmoid(conv_gate.astype(jnp.float32))).astype(
        jnp.bfloat16
    )
    taps = conv_kernel.shape[0]
    reach = (taps - 1) // 2
    length = gated.shape[1]
    padded = extended(gated, (("ep", 1),), reach).astype(jnp.float32)
    kernel_f = conv_kernel.astype(jnp.float32)
    summed = jnp.zeros(gated.shape, jnp.float32)
    for offset in range(taps):
        summed = summed + kernel_f[offset][:, None] * padded[:, offset : offset + length]
    conv_out = summed.astype(jnp.bfloat16)
    experts = lax.axis_size("ep")
    flat = expert_ids.reshape(-1)
    onehot = (flat[:, None] == jnp.arange(experts, dtype=jnp.int32)[None, :]).astype(jnp.int32)
    before = jnp.cumsum(onehot, axis=0) - onehot
    slots = flat.shape[0] // experts
    position = flat * slots + jnp.sum(before * onehot, axis=1)
    source_row = (
        jnp.zeros_like(flat).at[position].set(jnp.arange(flat.shape[0], dtype=jnp.int32) // 2)
    )
    slice_width = expert_input.shape[1] // lax.axis_size("tp")
    columns = lax.dynamic_slice_in_dim(
        expert_input, lax.axis_index("tp") * slice_width, slice_width, 1
    )
    sliced = lax.all_to_all(columns[source_row], "ep", split_axis=0, concat_axis=0, tiled=True)
    arrived = lax.all_gather(sliced, "tp", axis=1, tiled=True)
    gate_val = jnp.dot(arrived, expert_gate[0], preferred_element_type=jnp.float32)
    up_val = jnp.dot(arrived, expert_up[0], preferred_element_type=jnp.float32)
    hidden = (jax.nn.silu(gate_val) * up_val).astype(jnp.bfloat16)
    down_local = expert_down[0]
    whole_conv = lax.all_gather(conv_out, "tp", axis=0, tiled=True)
    produced = jnp.dot(
        lax.all_gather(hidden, "tp", axis=1, tiled=True),
        down_local,
        preferred_element_type=jnp.float32,
    )
    returned = lax.all_to_all(
        produced.astype(jnp.bfloat16), "ep", split_axis=0, concat_axis=0, tiled=True
    )
    copies = returned[position].reshape(-1, 2, returned.shape[1]).astype(jnp.float32)
    weights = route_weights(pair_logits, group_prob)
    expert_out = jnp.sum(copies * weights[:, :, None], axis=1).astype(jnp.bfloat16)
    swished = norm_swish(whole_conv, norm_gain, norm_shift)
    mixer_out = lax.dot_general(
        swished, out_weight, (((0,), (0,)), ((), ())), preferred_element_type=jnp.float32
    ).astype(jnp.bfloat16)
    return (mixer_out, expert_out)


GROUPS = 4


def swapped(cells, axis, step):
    return lax.ppermute(cells, axis, [(i, i ^ step) for i in range(lax.axis_size(axis))])


def shifted(cells, team, step):
    count = lax.axis_size("ep")
    return lax.ppermute(cells, "ep", [(i, (i + step * team) % count) for i in range(count)])


def in_order(mine, other, first, axis):
    low = jnp.where(first, mine, other)
    high = jnp.where(first, other, mine)
    return jnp.concatenate([low, high], axis=axis)


def thirds(values):
    parts = []
    for _ in range(3):
        part = lax.reduce_precision(values, 8, 7)
        parts.append(part.astype(jnp.bfloat16))
        values = values - part
    return parts


def paired(
    conv_value,
    conv_gate,
    conv_kernel,
    norm_gain,
    norm_shift,
    out_weight,
    expert_input,
    expert_ids,
    pair_logits,
    group_prob,
    expert_gate,
    expert_up,
    expert_down,
):
    team = lax.axis_size("ep") // GROUPS
    lanes = 128
    tokens = expert_input.shape[0]
    share = tokens // GROUPS
    place = lax.axis_index("ep")
    own_group = place // team
    own_first = place % team == 0
    spot = lax.axis_index("tp")
    core_first = spot % 2 == 0
    chip_first = spot // 2 == 0

    group = (expert_ids[:, 0] // team - own_group) % GROUPS
    counted = jnp.arange(tokens, dtype=jnp.int32)
    ahead = (group[:, None] == group[None, :]) & (counted[None, :] < counted[:, None])
    position = group * share + jnp.sum(ahead.astype(jnp.int32), axis=1)
    pick = (position[None, :] == counted[:, None]).astype(jnp.bfloat16)
    weights = route_weights(pair_logits, group_prob)
    straight = expert_ids[:, 0] % team == 0
    by_member = thirds(jnp.where(straight, weights[:, 0], weights[:, 1])) + thirds(
        jnp.where(straight, weights[:, 1], weights[:, 0])
    )
    extra = jnp.pad(jnp.stack(by_member, axis=1), ((0, 0), (0, lanes - len(by_member))))
    half = expert_input.shape[1] // 2
    columns = lax.dynamic_slice_in_dim(expert_input, (spot % 2) * half, half, 1)
    payload = jnp.dot(
        pick, jnp.concatenate([columns, extra], axis=1), preferred_element_type=jnp.float32
    ).astype(jnp.bfloat16)
    blocks = [payload[:share]]
    for step in range(1, GROUPS):
        blocks.append(shifted(payload[step * share : (step + 1) * share], team, step))
    across = [swapped(block[:, :half], "ep", 1) for block in blocks]
    came = jnp.concatenate(blocks, axis=0)
    mine_a = came[:, :half]
    other_a = swapped(mine_a, "tp", 1)
    mine_b = jnp.concatenate(across, axis=0)
    other_b = swapped(mine_b, "tp", 1)
    arrived = jnp.concatenate(
        [in_order(mine_a, other_a, core_first, 1), in_order(mine_b, other_b, core_first, 1)], axis=0
    )

    gated = (conv_value.astype(jnp.float32) * jax.nn.sigmoid(conv_gate.astype(jnp.float32))).astype(
        jnp.bfloat16
    )
    taps = conv_kernel.shape[0]
    reach = (taps - 1) // 2
    length = gated.shape[1]
    padded = extended(gated, (("ep", 1),), reach).astype(jnp.float32)
    kernel_f = conv_kernel.astype(jnp.float32)
    summed = jnp.zeros(gated.shape, jnp.float32)
    for offset in range(taps):
        summed = summed + kernel_f[offset][:, None] * padded[:, offset : offset + length]
    conv_out = summed.astype(jnp.bfloat16)
    far = swapped(conv_out, "tp", 2)
    near = swapped(conv_out, "tp", 1)
    both = swapped(far, "tp", 1)
    same_chip = in_order(conv_out, near, core_first, 0)
    other_chip = in_order(far, both, core_first, 0)
    whole_conv = in_order(same_chip, other_chip, chip_first, 0)
    swished = norm_swish(whole_conv, norm_gain, norm_shift)
    mixer_out = lax.dot_general(
        swished, out_weight, (((0,), (0,)), ((), ())), preferred_element_type=jnp.float32
    ).astype(jnp.bfloat16)

    gate_val = jnp.dot(arrived, expert_gate[0], preferred_element_type=jnp.float32)
    up_val = jnp.dot(arrived, expert_up[0], preferred_element_type=jnp.float32)
    hidden = (jax.nn.silu(gate_val) * up_val).astype(jnp.bfloat16)
    hidden_far = swapped(hidden, "tp", 2)
    hidden_near = swapped(hidden, "tp", 1)
    hidden_both = swapped(hidden_far, "tp", 1)
    whole_hidden = in_order(
        in_order(hidden, hidden_near, core_first, 1),
        in_order(hidden_far, hidden_both, core_first, 1),
        chip_first,
        1,
    )
    produced = jnp.dot(whole_hidden, expert_down[0], preferred_element_type=jnp.float32).astype(
        jnp.bfloat16
    )
    given = swapped(produced[tokens:], "ep", 1)
    carried = came[:, half:].astype(jnp.float32)
    for_low = carried[:, 0:1] + carried[:, 1:2] + carried[:, 2:3]
    for_high = carried[:, 3:4] + carried[:, 4:5] + carried[:, 5:6]
    weight_mine = jnp.where(own_first, for_low, for_high)
    weight_other = jnp.where(own_first, for_high, for_low)
    joined = (
        produced[:tokens].astype(jnp.float32) * weight_mine + given.astype(jnp.float32) * weight_other
    ).astype(jnp.bfloat16)
    back = [joined[:share]]
    for step in range(1, GROUPS):
        back.append(shifted(joined[step * share : (step + 1) * share], team, -step))
    expert_out = lax.dot_general(
        pick,
        jnp.concatenate(back, axis=0),
        (((0,), (0,)), ((), ())),
        preferred_element_type=jnp.float32,
    ).astype(jnp.bfloat16)
    return (mixer_out, expert_out)


def solution(mesh):
    plan = paired if mesh.shape["ep"] == 2 * GROUPS and mesh.shape["tp"] == 4 else local
    placed = (
        P("tp", "ep"),
        P("tp", "ep"),
        P(None, "tp"),
        P(),
        P(),
        P(None, "tp"),
        P("ep", None),
        P("ep", None),
        P("ep", None),
        P("ep"),
        P("ep", None, "tp"),
        P("ep", None, "tp"),
        P("ep", None, "tp"),
    )
    return jax.shard_map(
        plan, mesh=mesh, in_specs=placed, out_specs=(P("ep", "tp"), P("ep", "tp")), check_vma=False
    )
```

```python
import jax
import jax.numpy as jnp
from jax import lax
from jax.experimental import pallas as pl
from jax.experimental.pallas import tpu as pltpu
from jax.sharding import PartitionSpec as P


def extended(cells, sides, width):
    for axis, dim in sides:
        count = lax.axis_size(axis)
        ends = count - 1
        head = lax.slice_in_dim(cells, 0, width, axis=dim)
        tail = lax.slice_in_dim(cells, cells.shape[dim] - width, cells.shape[dim], axis=dim)
        cells = jnp.concatenate(
            [
                lax.ppermute(tail, axis, [(i, (i + 1) % count) for i in range(ends)]),
                cells,
                lax.ppermute(head, axis, [((i + 1) % count, i) for i in range(ends)]),
            ],
            axis=dim,
        )
    return cells


def norm_swish(conv_out, norm_gain, norm_shift):
    values = conv_out.astype(jnp.float32)
    center = jnp.mean(values, axis=0, keepdims=True)
    spread = jnp.mean(jnp.square(values - center), axis=0, keepdims=True)
    normed = (values - center) * lax.rsqrt(spread + 1e-05) * norm_gain[:, None] + norm_shift[
        :, None
    ]
    return jax.nn.silu(normed).astype(jnp.bfloat16)


def route_weights(pair_logits, group_prob):
    share = jax.nn.sigmoid(pair_logits[:, 0] - pair_logits[:, 1])
    return jnp.stack([share, 1.0 - share], axis=1) * group_prob[:, None]


def local(
    conv_value,
    conv_gate,
    conv_kernel,
    norm_gain,
    norm_shift,
    out_weight,
    expert_input,
    expert_ids,
    pair_logits,
    group_prob,
    expert_gate,
    expert_up,
    expert_down,
):
    gated = (conv_value.astype(jnp.float32) * jax.nn.sigmoid(conv_gate.astype(jnp.float32))).astype(
        jnp.bfloat16
    )
    taps = conv_kernel.shape[0]
    reach = (taps - 1) // 2
    length = gated.shape[1]
    padded = extended(gated, (("ep", 1),), reach).astype(jnp.float32)
    kernel_f = conv_kernel.astype(jnp.float32)
    summed = jnp.zeros(gated.shape, jnp.float32)
    for offset in range(taps):
        summed = summed + kernel_f[offset][:, None] * padded[:, offset : offset + length]
    conv_out = summed.astype(jnp.bfloat16)
    experts = lax.axis_size("ep")
    flat = expert_ids.reshape(-1)
    onehot = (flat[:, None] == jnp.arange(experts, dtype=jnp.int32)[None, :]).astype(jnp.int32)
    before = jnp.cumsum(onehot, axis=0) - onehot
    slots = flat.shape[0] // experts
    position = flat * slots + jnp.sum(before * onehot, axis=1)
    source_row = (
        jnp.zeros_like(flat).at[position].set(jnp.arange(flat.shape[0], dtype=jnp.int32) // 2)
    )
    slice_width = expert_input.shape[1] // lax.axis_size("tp")
    columns = lax.dynamic_slice_in_dim(
        expert_input, lax.axis_index("tp") * slice_width, slice_width, 1
    )
    sliced = lax.all_to_all(columns[source_row], "ep", split_axis=0, concat_axis=0, tiled=True)
    arrived = lax.all_gather(sliced, "tp", axis=1, tiled=True)
    gate_val = jnp.dot(arrived, expert_gate[0], preferred_element_type=jnp.float32)
    up_val = jnp.dot(arrived, expert_up[0], preferred_element_type=jnp.float32)
    hidden = (jax.nn.silu(gate_val) * up_val).astype(jnp.bfloat16)
    down_local = expert_down[0]
    whole_conv = lax.all_gather(conv_out, "tp", axis=0, tiled=True)
    produced = jnp.dot(
        lax.all_gather(hidden, "tp", axis=1, tiled=True),
        down_local,
        preferred_element_type=jnp.float32,
    )
    returned = lax.all_to_all(
        produced.astype(jnp.bfloat16), "ep", split_axis=0, concat_axis=0, tiled=True
    )
    copies = returned[position].reshape(-1, 2, returned.shape[1]).astype(jnp.float32)
    weights = route_weights(pair_logits, group_prob)
    expert_out = jnp.sum(copies * weights[:, :, None], axis=1).astype(jnp.bfloat16)
    swished = norm_swish(whole_conv, norm_gain, norm_shift)
    mixer_out = lax.dot_general(
        swished, out_weight, (((0,), (0,)), ((), ())), preferred_element_type=jnp.float32
    ).astype(jnp.bfloat16)
    return (mixer_out, expert_out)


GROUPS = 4


def swapped(cells, axis, step):
    return lax.ppermute(cells, axis, [(i, i ^ step) for i in range(lax.axis_size(axis))])


def shifted(cells, team, step):
    count = lax.axis_size("ep")
    return lax.ppermute(cells, "ep", [(i, (i + step * team) % count) for i in range(count)])


def in_order(mine, other, first, axis):
    low = jnp.where(first, mine, other)
    high = jnp.where(first, other, mine)
    return jnp.concatenate([low, high], axis=axis)


def thirds(values):
    parts = []
    for _ in range(3):
        part = values.astype(jnp.bfloat16).astype(jnp.float32)
        parts.append(part)
        values = values - part
    return parts


def route_body(team, numbers, ids, logits, prob, cells, *outs):
    blocks, pick_out = outs[:-1], outs[-1]
    tokens, half = cells.shape
    share = tokens // GROUPS
    first = ids[:, 0:1]
    group = first // team - numbers[1]
    group = jnp.where(group < 0, group + GROUPS, group)
    down = lax.broadcasted_iota(jnp.int32, (tokens, tokens), 0)
    right = lax.broadcasted_iota(jnp.int32, (tokens, tokens), 1)
    group_row = jnp.sum(jnp.where(down == right, group, 0), axis=0, keepdims=True)
    ahead = jnp.where((group == group_row) & (right < down), 1, 0)
    position = group * share + jnp.sum(ahead, axis=1, keepdims=True)
    position_row = jnp.sum(jnp.where(down == right, position, 0), axis=0, keepdims=True)
    pick = jnp.where(position_row == down, 1.0, 0.0).astype(jnp.bfloat16)
    pick_out[...] = pick
    share_0 = jax.nn.sigmoid(logits[:, 0:1] - logits[:, 1:2])
    weight_0 = share_0 * prob[...]
    weight_1 = (1.0 - share_0) * prob[...]
    straight = first - (first // team) * team == 0
    parts = thirds(jnp.where(straight, weight_0, weight_1)) + thirds(
        jnp.where(straight, weight_1, weight_0)
    )
    lane = lax.broadcasted_iota(jnp.int32, (tokens, 128), 1)
    extra = jnp.zeros((tokens, 128), jnp.float32)
    for at, part in enumerate(parts):
        extra = jnp.where(lane == at, part, extra)
    moved = jnp.dot(pick, cells[...], preferred_element_type=jnp.float32).astype(jnp.bfloat16)
    carried = jnp.dot(
        pick, extra.astype(jnp.bfloat16), preferred_element_type=jnp.float32
    ).astype(jnp.bfloat16)
    for at, block in enumerate(blocks):
        block[:, :half] = moved[at * share : (at + 1) * share]
        block[:, half:] = carried[at * share : (at + 1) * share]


def route(numbers, expert_ids, pair_logits, group_prob, expert_input, team):
    tokens, width = expert_input.shape
    half = width // 2
    share = tokens // GROUPS

    def whole(shape):
        return pl.BlockSpec(shape, lambda i, n: (0, 0))

    block = (share, half + 128)
    return pl.pallas_call(
        lambda *refs: route_body(team, *refs),
        grid_spec=pltpu.PrefetchScalarGridSpec(
            num_scalar_prefetch=1,
            grid=(1,),
            in_specs=[
                whole((tokens, 2)),
                whole((tokens, 2)),
                whole((tokens, 1)),
                pl.BlockSpec((tokens, half), lambda i, n: (0, n[0])),
            ],
            out_specs=[whole(block)] * GROUPS + [whole((tokens, tokens))],
        ),
        out_shape=[jax.ShapeDtypeStruct(block, jnp.bfloat16)] * GROUPS
        + [jax.ShapeDtypeStruct((tokens, tokens), jnp.bfloat16)],
    )(numbers, expert_ids, pair_logits, group_prob[:, None], expert_input)


def paired(
    conv_value,
    conv_gate,
    conv_kernel,
    norm_gain,
    norm_shift,
    out_weight,
    expert_input,
    expert_ids,
    pair_logits,
    group_prob,
    expert_gate,
    expert_up,
    expert_down,
):
    team = lax.axis_size("ep") // GROUPS
    tokens = expert_input.shape[0]
    share = tokens // GROUPS
    half = expert_input.shape[1] // 2
    place = lax.axis_index("ep")
    own_first = place % team == 0
    spot = lax.axis_index("tp")
    core_first = spot % 2 == 0
    chip_first = spot // 2 == 0

    gated = (conv_value.astype(jnp.float32) * jax.nn.sigmoid(conv_gate.astype(jnp.float32))).astype(
        jnp.bfloat16
    )
    taps = conv_kernel.shape[0]
    reach = (taps - 1) // 2
    length = gated.shape[1]
    padded = extended(gated, (("ep", 1),), reach)

    numbers = jnp.stack([spot % 2, place // team]).astype(jnp.int32)
    *sent, pick = route(numbers, expert_ids, pair_logits, group_prob, expert_input, team)
    padded, sent = lax.optimization_barrier((padded, sent))
    blocks = [sent[0]]
    for step in range(1, GROUPS):
        blocks.append(shifted(sent[step], team, step))
    across = []
    for block in blocks:
        across.append(swapped(block[:, :half], "ep", 1))
    came = jnp.concatenate(blocks, axis=0)

    padded = padded.astype(jnp.float32)
    kernel_f = conv_kernel.astype(jnp.float32)
    summed = jnp.zeros(gated.shape, jnp.float32)
    for offset in range(taps):
        summed = summed + kernel_f[offset][:, None] * padded[:, offset : offset + length]
    conv_out = summed.astype(jnp.bfloat16)
    conv_out = lax.optimization_barrier(conv_out)

    def gathered(cells, axis):
        far = swapped(cells, "tp", 2)
        near = swapped(cells, "tp", 1)
        both = swapped(far, "tp", 1)
        same_chip = in_order(cells, near, core_first, axis)
        other_chip = in_order(far, both, core_first, axis)
        return in_order(same_chip, other_chip, chip_first, axis)

    swished = norm_swish(gathered(conv_out, 0), norm_gain, norm_shift)
    mixer_out = lax.dot_general(
        swished, out_weight, (((0,), (0,)), ((), ())), preferred_element_type=jnp.float32
    ).astype(jnp.bfloat16)

    def hidden_of(mine):
        rows = in_order(mine, swapped(mine, "tp", 1), core_first, 1)
        gate_val = jnp.dot(rows, expert_gate[0], preferred_element_type=jnp.float32)
        up_val = jnp.dot(rows, expert_up[0], preferred_element_type=jnp.float32)
        hidden = (jax.nn.silu(gate_val) * up_val).astype(jnp.bfloat16)
        return gathered(lax.optimization_barrier(hidden), 1)

    hidden_a = hidden_of(came[:, :half])
    hidden_b = hidden_of(jnp.concatenate(across, axis=0))
    produced_b = jnp.dot(hidden_b, expert_down[0], preferred_element_type=jnp.float32).astype(
        jnp.bfloat16
    )
    produced_a = jnp.dot(hidden_a, expert_down[0], preferred_element_type=jnp.float32).astype(
        jnp.bfloat16
    )
    carried = came[:, half:].astype(jnp.float32)
    for_low = carried[:, 0:1] + carried[:, 1:2] + carried[:, 2:3]
    for_high = carried[:, 3:4] + carried[:, 4:5] + carried[:, 5:6]
    weight_mine = jnp.where(own_first, for_low, for_high)
    weight_other = jnp.where(own_first, for_high, for_low)

    def joined(low, high):
        given = swapped(produced_b[low:high], "ep", 1)
        return (
            produced_a[low:high].astype(jnp.float32) * weight_mine[low:high]
            + given.astype(jnp.float32) * weight_other[low:high]
        ).astype(jnp.bfloat16)

    early = joined(share, 3 * share)
    back = [shifted(early[:share], team, -1), shifted(early[share:], team, -2)]
    last = joined(3 * share, 4 * share)
    back.append(shifted(last, team, -3))
    back.insert(0, joined(0, share))
    expert_out = lax.dot_general(
        pick,
        jnp.concatenate(back, axis=0),
        (((0,), (0,)), ((), ())),
        preferred_element_type=jnp.float32,
    ).astype(jnp.bfloat16)
    return (mixer_out, expert_out)


def solution(mesh):
    plan = paired if mesh.shape["ep"] == 2 * GROUPS and mesh.shape["tp"] == 4 else local
    placed = (
        P("tp", "ep"),
        P("tp", "ep"),
        P(None, "tp"),
        P(),
        P(),
        P(None, "tp"),
        P("ep", None),
        P("ep", None),
        P("ep", None),
        P("ep"),
        P("ep", None, "tp"),
        P("ep", None, "tp"),
        P("ep", None, "tp"),
    )
    return jax.shard_map(
        plan, mesh=mesh, in_specs=placed, out_specs=(P("ep", "tp"), P("ep", "tp")), check_vma=False
    )
```

```python
import jax
import jax.numpy as jnp
from jax import lax
from jax.experimental import pallas as pl
from jax.experimental.pallas import tpu as pltpu
from jax.sharding import PartitionSpec as P


def extended(cells, sides, width):
    for axis, dim in sides:
        count = lax.axis_size(axis)
        ends = count - 1
        head = lax.slice_in_dim(cells, 0, width, axis=dim)
        tail = lax.slice_in_dim(cells, cells.shape[dim] - width, cells.shape[dim], axis=dim)
        cells = jnp.concatenate(
            [
                lax.ppermute(tail, axis, [(i, (i + 1) % count) for i in range(ends)]),
                cells,
                lax.ppermute(head, axis, [((i + 1) % count, i) for i in range(ends)]),
            ],
            axis=dim,
        )
    return cells


def norm_swish(conv_out, norm_gain, norm_shift):
    values = conv_out.astype(jnp.float32)
    center = jnp.mean(values, axis=0, keepdims=True)
    spread = jnp.mean(jnp.square(values - center), axis=0, keepdims=True)
    normed = (values - center) * lax.rsqrt(spread + 1e-05) * norm_gain[:, None] + norm_shift[
        :, None
    ]
    return jax.nn.silu(normed).astype(jnp.bfloat16)


def route_weights(pair_logits, group_prob):
    share = jax.nn.sigmoid(pair_logits[:, 0] - pair_logits[:, 1])
    return jnp.stack([share, 1.0 - share], axis=1) * group_prob[:, None]


def local(
    conv_value,
    conv_gate,
    conv_kernel,
    norm_gain,
    norm_shift,
    out_weight,
    expert_input,
    expert_ids,
    pair_logits,
    group_prob,
    expert_gate,
    expert_up,
    expert_down,
):
    gated = (conv_value.astype(jnp.float32) * jax.nn.sigmoid(conv_gate.astype(jnp.float32))).astype(
        jnp.bfloat16
    )
    taps = conv_kernel.shape[0]
    reach = (taps - 1) // 2
    length = gated.shape[1]
    padded = extended(gated, (("ep", 1),), reach).astype(jnp.float32)
    kernel_f = conv_kernel.astype(jnp.float32)
    summed = jnp.zeros(gated.shape, jnp.float32)
    for offset in range(taps):
        summed = summed + kernel_f[offset][:, None] * padded[:, offset : offset + length]
    conv_out = summed.astype(jnp.bfloat16)
    experts = lax.axis_size("ep")
    flat = expert_ids.reshape(-1)
    onehot = (flat[:, None] == jnp.arange(experts, dtype=jnp.int32)[None, :]).astype(jnp.int32)
    before = jnp.cumsum(onehot, axis=0) - onehot
    slots = flat.shape[0] // experts
    position = flat * slots + jnp.sum(before * onehot, axis=1)
    source_row = (
        jnp.zeros_like(flat).at[position].set(jnp.arange(flat.shape[0], dtype=jnp.int32) // 2)
    )
    slice_width = expert_input.shape[1] // lax.axis_size("tp")
    columns = lax.dynamic_slice_in_dim(
        expert_input, lax.axis_index("tp") * slice_width, slice_width, 1
    )
    sliced = lax.all_to_all(columns[source_row], "ep", split_axis=0, concat_axis=0, tiled=True)
    arrived = lax.all_gather(sliced, "tp", axis=1, tiled=True)
    gate_val = jnp.dot(arrived, expert_gate[0], preferred_element_type=jnp.float32)
    up_val = jnp.dot(arrived, expert_up[0], preferred_element_type=jnp.float32)
    hidden = (jax.nn.silu(gate_val) * up_val).astype(jnp.bfloat16)
    down_local = expert_down[0]
    whole_conv = lax.all_gather(conv_out, "tp", axis=0, tiled=True)
    produced = jnp.dot(
        lax.all_gather(hidden, "tp", axis=1, tiled=True),
        down_local,
        preferred_element_type=jnp.float32,
    )
    returned = lax.all_to_all(
        produced.astype(jnp.bfloat16), "ep", split_axis=0, concat_axis=0, tiled=True
    )
    copies = returned[position].reshape(-1, 2, returned.shape[1]).astype(jnp.float32)
    weights = route_weights(pair_logits, group_prob)
    expert_out = jnp.sum(copies * weights[:, :, None], axis=1).astype(jnp.bfloat16)
    swished = norm_swish(whole_conv, norm_gain, norm_shift)
    mixer_out = lax.dot_general(
        swished, out_weight, (((0,), (0,)), ((), ())), preferred_element_type=jnp.float32
    ).astype(jnp.bfloat16)
    return (mixer_out, expert_out)


GROUPS = 4


def swapped(cells, axis, step):
    return lax.ppermute(cells, axis, [(i, i ^ step) for i in range(lax.axis_size(axis))])


def shifted(cells, team, step):
    count = lax.axis_size("ep")
    return lax.ppermute(cells, "ep", [(i, (i + step * team) % count) for i in range(count)])


def in_order(mine, other, first, axis):
    low = jnp.where(first, mine, other)
    high = jnp.where(first, other, mine)
    return jnp.concatenate([low, high], axis=axis)


def thirds(values):
    parts = []
    for _ in range(3):
        part = values.astype(jnp.bfloat16).astype(jnp.float32)
        parts.append(part)
        values = values - part
    return parts


def route_body(team, numbers, ids, logits, prob, cells, *outs):
    own, own_extra, *blocks, pick_out = outs
    tokens, half = cells.shape
    share = tokens // GROUPS
    first = ids[0:1, :]
    group_row = first // team - numbers[1]
    group_row = jnp.where(group_row < 0, group_row + GROUPS, group_row)
    down = lax.broadcasted_iota(jnp.int32, (tokens, tokens), 0)
    right = lax.broadcasted_iota(jnp.int32, (tokens, tokens), 1)
    group = jnp.sum(jnp.where(down == right, group_row, 0), axis=1, keepdims=True)
    ahead = jnp.where((group == group_row) & (down < right), 1, 0)
    position_row = group_row * share + jnp.sum(ahead, axis=0, keepdims=True)
    pick = jnp.where(position_row == down, 1.0, 0.0).astype(jnp.bfloat16)
    pick_out[...] = pick
    share_0 = jax.nn.sigmoid(logits[0:1, :] - logits[1:2, :])
    weight_0 = share_0 * prob[...]
    weight_1 = (1.0 - share_0) * prob[...]
    straight = first - (first // team) * team == 0
    parts = thirds(jnp.where(straight, weight_0, weight_1)) + thirds(
        jnp.where(straight, weight_1, weight_0)
    )
    line = lax.broadcasted_iota(jnp.int32, (128, tokens), 0)
    extra = jnp.zeros((128, tokens), jnp.float32)
    for at, part in enumerate(parts):
        extra = jnp.where(line == at, part, extra)
    moved = jnp.dot(pick, cells[...], preferred_element_type=jnp.float32).astype(jnp.bfloat16)
    carried = lax.dot_general(
        pick,
        extra.astype(jnp.bfloat16),
        (((1,), (1,)), ((), ())),
        preferred_element_type=jnp.float32,
    ).astype(jnp.bfloat16)
    own[...] = moved[:share]
    own_extra[...] = carried[:share]
    for at, block in enumerate(blocks, 1):
        block[:, :half] = moved[at * share : (at + 1) * share]
        block[:, half:] = carried[at * share : (at + 1) * share]


def route(numbers, expert_ids, pair_logits, group_prob, expert_input, team):
    tokens, width = expert_input.shape
    half = width // 2
    share = tokens // GROUPS

    def whole(shape):
        return pl.BlockSpec(shape, lambda i, n: (0, 0))

    block = (share, half + 128)
    shapes = [(share, half), (share, 128)] + [block] * (GROUPS - 1) + [(tokens, tokens)]
    return pl.pallas_call(
        lambda *refs: route_body(team, *refs),
        grid_spec=pltpu.PrefetchScalarGridSpec(
            num_scalar_prefetch=1,
            grid=(1,),
            in_specs=[
                whole((2, tokens)),
                whole((2, tokens)),
                whole((1, tokens)),
                pl.BlockSpec((tokens, half), lambda i, n: (0, n[0])),
            ],
            out_specs=[whole(shape) for shape in shapes],
        ),
        out_shape=[jax.ShapeDtypeStruct(shape, jnp.bfloat16) for shape in shapes],
    )(numbers, expert_ids.T, pair_logits.T, group_prob[None, :], expert_input)


def paired(
    conv_value,
    conv_gate,
    conv_kernel,
    norm_gain,
    norm_shift,
    out_weight,
    expert_input,
    expert_ids,
    pair_logits,
    group_prob,
    expert_gate,
    expert_up,
    expert_down,
):
    team = lax.axis_size("ep") // GROUPS
    tokens = expert_input.shape[0]
    share = tokens // GROUPS
    half = expert_input.shape[1] // 2
    place = lax.axis_index("ep")
    own_first = place % team == 0
    spot = lax.axis_index("tp")
    core_first = spot % 2 == 0
    chip_first = spot // 2 == 0

    gated = (conv_value.astype(jnp.float32) * jax.nn.sigmoid(conv_gate.astype(jnp.float32))).astype(
        jnp.bfloat16
    )
    taps = conv_kernel.shape[0]
    reach = (taps - 1) // 2
    length = gated.shape[1]
    padded = extended(gated, (("ep", 1),), reach)

    numbers = jnp.stack([spot % 2, place // team]).astype(jnp.int32)
    *sent, pick = route(numbers, expert_ids, pair_logits, group_prob, expert_input, team)
    padded, sent, conv_kernel = lax.optimization_barrier((padded, sent, conv_kernel))
    own, own_extra, *sent = sent
    arrivals = []
    for step, block in enumerate(sent, 1):
        arrivals.append(shifted(block, team, step))
    blocks = [own] + [block[:, :half] for block in arrivals]
    across = []
    for block in blocks:
        across.append(swapped(block, "ep", 1))

    kernel_f = conv_kernel.astype(jnp.float32)
    tap = [kernel_f[offset][:, None] for offset in range(taps)]
    pieces = []
    wide = length // 2
    for piece in range(2):
        window = padded[:, piece * wide : (piece + 1) * wide + taps - 1].astype(jnp.float32)
        summed = jnp.zeros((gated.shape[0], wide), jnp.float32)
        for offset in range(taps):
            summed = summed + tap[offset] * window[:, offset : offset + wide]
        pieces.append(lax.optimization_barrier(summed.astype(jnp.bfloat16)))
    conv_out = lax.optimization_barrier(jnp.concatenate(pieces, axis=1))

    def gathered(cells, axis):
        far = swapped(cells, "tp", 2)
        near = swapped(cells, "tp", 1)
        both = swapped(far, "tp", 1)
        same_chip = in_order(cells, near, core_first, axis)
        other_chip = in_order(far, both, core_first, axis)
        return in_order(same_chip, other_chip, chip_first, axis)

    swished = norm_swish(gathered(conv_out, 0), norm_gain, norm_shift)
    mixer_out = lax.dot_general(
        swished, out_weight, (((0,), (0,)), ((), ())), preferred_element_type=jnp.float32
    ).astype(jnp.bfloat16)

    def hidden_of(mine):
        rows = in_order(mine, swapped(mine, "tp", 1), core_first, 1)
        gate_val = jnp.dot(rows, expert_gate[0], preferred_element_type=jnp.float32)
        up_val = jnp.dot(rows, expert_up[0], preferred_element_type=jnp.float32)
        hidden = (jax.nn.silu(gate_val) * up_val).astype(jnp.bfloat16)
        return gathered(lax.optimization_barrier(hidden), 1)

    hidden_a = hidden_of(jnp.concatenate(blocks, axis=0))
    hidden_b = hidden_of(jnp.concatenate(across, axis=0))
    produced_b = jnp.dot(hidden_b, expert_down[0], preferred_element_type=jnp.float32).astype(
        jnp.bfloat16
    )
    produced_a = jnp.dot(hidden_a, expert_down[0], preferred_element_type=jnp.float32).astype(
        jnp.bfloat16
    )
    carried = jnp.concatenate([own_extra] + [block[:, half:] for block in arrivals], axis=0)
    carried = carried.astype(jnp.float32)
    for_low = carried[:, 0:1] + carried[:, 1:2] + carried[:, 2:3]
    for_high = carried[:, 3:4] + carried[:, 4:5] + carried[:, 5:6]
    weight_mine = jnp.where(own_first, for_low, for_high)
    weight_other = jnp.where(own_first, for_high, for_low)

    def joined(low, high):
        given = swapped(produced_b[low:high], "ep", 1)
        return (
            produced_a[low:high].astype(jnp.float32) * weight_mine[low:high]
            + given.astype(jnp.float32) * weight_other[low:high]
        ).astype(jnp.bfloat16)

    early = joined(share, 3 * share)
    back = [shifted(early[:share], team, -1), shifted(early[share:], team, -2)]
    last = joined(3 * share, 4 * share)
    back.append(shifted(last, team, -3))
    back.insert(0, joined(0, share))
    expert_out = lax.dot_general(
        pick,
        jnp.concatenate(back, axis=0),
        (((0,), (0,)), ((), ())),
        preferred_element_type=jnp.float32,
    ).astype(jnp.bfloat16)
    return (mixer_out, expert_out)


def solution(mesh):
    plan = paired if mesh.shape["ep"] == 2 * GROUPS and mesh.shape["tp"] == 4 else local
    placed = (
        P("tp", "ep"),
        P("tp", "ep"),
        P(None, "tp"),
        P(),
        P(),
        P(None, "tp"),
        P("ep", None),
        P("ep", None),
        P("ep", None),
        P("ep"),
        P("ep", None, "tp"),
        P("ep", None, "tp"),
        P("ep", None, "tp"),
    )
    return jax.shard_map(
        plan, mesh=mesh, in_specs=placed, out_specs=(P("ep", "tp"), P("ep", "tp")), check_vma=False
    )
```
